32 devices in a mesh: sp: 4 (over y, x), tp: 8 (over z, core).
Axes of the slice: x: 2, y: 2, z: 4, core: 2. Of those that a mesh axis runs over, the one named last changes fastest.
Arguments:
- tokens: bfloat16 [2, 512, 4096], P(None, 'sp', 'tp'), may hold values from -6 to 6
- key_matrix: bfloat16 [4096, 4096], P(None, 'tp'), may hold values from -0.09375 to 0.09375
- value_matrix: bfloat16 [4096, 4096], P(None, 'tp'), may hold values from -0.375 to 0.375
- gate_matrix: bfloat16 [4096, 64], replicated, may hold values from -0.09375 to 0.09375
- head_decay_rate: float32 [32], P('tp'), may hold values from 0 to 1, as said below
- extra_log_decay: float32 [2, 32, 512], P(None, 'tp', 'sp'), may hold values from -3 to 0, as said below
- next_token_query: bfloat16 [2, 4096], P(None, 'tp'), may hold values from -6 to 6
- next_token_key: bfloat16 [2, 4096], P(None, 'tp'), may hold values from -6 to 6
- next_token_value: bfloat16 [2, 32, 128], P(None, 'tp', 'sp'), may hold values from -6 to 6
- next_write_strength: float32 [2, 32], P(None, 'tp'), may hold values from 0.05 to 1
- read_norm_gain: float32 [128], P('sp'), may hold values from 0.1 to 1.9
Outputs:
- state_cache: bfloat16 [2, 32, 128, 128], P(None, 'tp', None, 'sp')
- first_read: bfloat16 [2, 32, 128], P(None, 'tp', 'sp')
The draws below stay inside these ranges and needn't reach their ends.
Inputs may be any that keep to these rules, and one draw needn't show every extreme that they name: `head_decay_rate`: positive. `extra_log_decay`: never positive.
All inputs are finite; a program needn't handle non-finite values.
Results may differ from the reference program's by a relative error of at most 0.013.
Values may be sent and summed in bfloat16 or wider, within the bound.
A program may use at most 64 MiB of HBM per device.

```python
import jax
import jax.numpy as jnp
from jax import lax

D = 4096
HEAD_COUNT = 32
DK = 128
DV = 128
PROMPT_COUNT = 2
POS_DEV = 128
BLOCK = 64
PROMPT_LENGTH = 512


def draw_head_decay_rate(key, part):
    chooser, fast_key, slow_key = jax.random.split(jax.random.fold_in(key, 11), 3)
    fast_share = 0.5
    fast_mask = jax.random.uniform(chooser, (HEAD_COUNT,), jnp.float32) < fast_share
    fast_rate = jnp.exp(jax.random.uniform(fast_key, (HEAD_COUNT,), jnp.float32, jnp.log(0.02), jnp.log(0.05)))
    slow_rate = jnp.exp(jax.random.uniform(slow_key, (HEAD_COUNT,), jnp.float32, jnp.log(0.05 / PROMPT_LENGTH), jnp.log(0.4 / PROMPT_LENGTH)))
    return jnp.where(fast_mask, fast_rate, slow_rate).astype(jnp.float32)


def draw_extra_log_decay(key, part):
    block_key, location_seed, magnitude_seed = jax.random.split(jax.random.fold_in(key, 23), 3)
    lowest_rate = 0.05
    highest_rate = 0.6
    block_total = PROMPT_LENGTH // POS_DEV
    block_rate = jnp.exp(jax.random.uniform(block_key, (PROMPT_COUNT, HEAD_COUNT, block_total), jnp.float32, jnp.log(lowest_rate / PROMPT_LENGTH), jnp.log(highest_rate / PROMPT_LENGTH)))
    position_decay = jnp.repeat(block_rate, POS_DEV, axis=2)
    spike_positions = jax.random.randint(location_seed, (PROMPT_COUNT, HEAD_COUNT, 2), 0, PROMPT_LENGTH)
    spike_magnitude = jnp.log(jax.random.uniform(magnitude_seed, (PROMPT_COUNT, HEAD_COUNT, 2), jnp.float32, 0.5, 0.8))
    spike_locations = jnp.arange(PROMPT_LENGTH, dtype=jnp.int32)
    decay_spikes = jnp.sum(jnp.where(spike_locations[None, None, None, :] == spike_positions[..., None], spike_magnitude[..., None], 0.0), axis=2)
    return (decay_spikes - position_decay).astype(jnp.float32)


def level_of(own_key, dims, shards, smallest, top_value):
    gain, own = 1.0, jax.random.fold_in(own_key, 6)
    for position, parts in shards:
        heights = jnp.exp(jax.random.uniform(jax.random.fold_in(own, position), (parts,), jnp.float32, smallest / len(shards), top_value / len(shards)))
        gain = gain * jnp.repeat(heights, dims[position] // parts).reshape([-1 if axis == position else 1 for axis in range(len(dims))])
    return gain


def bell_draw(own_key, shape, width, most, cuts=(), held_as=jnp.bfloat16):
    values = width * jax.random.normal(own_key, shape, jnp.float32)
    if cuts:
        values = values * level_of(own_key, shape, cuts, -0.22, 0.18)
    return jnp.clip(values, -most, most).astype(held_as)


def setup_inputs(seed: int = 0) -> dict:
    splits = jax.random.split(jax.random.key(seed), 12)
    return {
        "tokens": bell_draw(splits[0], (PROMPT_COUNT, PROMPT_LENGTH, D), 1.0, 6.0, ((1, 4), (2, 8))),
        "key_matrix": bell_draw(splits[1], (D, HEAD_COUNT * DK), D ** -0.5, 0.09375, ((1, 8),)),
        "value_matrix": bell_draw(splits[2], (D, HEAD_COUNT * DV), (D // 16) ** -0.5, 0.375, ((1, 8),)),
        "gate_matrix": bell_draw(splits[3], (D, 2 * HEAD_COUNT), D ** -0.5, 0.09375),
        "head_decay_rate": draw_head_decay_rate(jax.random.fold_in(splits[11], 71), 0),
        "extra_log_decay": draw_extra_log_decay(jax.random.fold_in(splits[11], 71), 0),
        "next_token_query": bell_draw(splits[6], (PROMPT_COUNT, HEAD_COUNT * DK), 1.0, 6.0, ((1, 8),)),
        "next_token_key": bell_draw(splits[7], (PROMPT_COUNT, HEAD_COUNT * DK), 1.0, 6.0, ((1, 8),)),
        "next_token_value": bell_draw(splits[8], (PROMPT_COUNT, HEAD_COUNT, DV), 1.0, 6.0, ((1, 8), (2, 4))),
        "next_write_strength": jnp.clip(0.05 + 0.95 * jax.random.uniform(splits[9], (PROMPT_COUNT, HEAD_COUNT), jnp.float32) ** level_of(splits[9], (PROMPT_COUNT, HEAD_COUNT), ((1, 8),), -0.2, 0.2), 0.05, 1.0),
        "read_norm_gain": jnp.clip(1.0 + 0.18 * jax.random.normal(splits[10], (DV,), jnp.float32), 0.1, 1.9),
    }


exact_mode = lax.Precision.HIGHEST
strength_offset = 5.0

def unit_rows(matrix):
    return matrix * lax.rsqrt(lax.optimization_barrier(jnp.sum(matrix * matrix, axis=-1, keepdims=True)) + 1e-06)

def nilpotent_inverse(mixing):
    extent = mixing.shape[-1]
    result = jnp.zeros_like(mixing) + jnp.eye(extent, dtype=jnp.float32)
    powered = -mixing
    covered = 1
    while covered < extent:
        result = result + jnp.einsum('...ij,...jk->...ik', result, powered, precision=exact_mode)
        powered = jnp.einsum('...ij,...jk->...ik', powered, powered, precision=exact_mode)
        covered = covered * 2
    return result

def block_terms(unit_keys, values, decay_logarithm, strength):
    extent = unit_keys.shape[-2]
    lower = jnp.tril(jnp.ones((extent, extent), jnp.bool_))
    strict = jnp.tril(jnp.ones((extent, extent), jnp.bool_), -1)
    running = jnp.cumsum(decay_logarithm, axis=-1)
    spread = running[..., :, None] - running[..., None, :]
    within = jnp.where(lower, jnp.exp(jnp.where(lower, spread, 0.0)), 0.0)
    scaled = unit_keys * strength[..., None]
    mixing = jnp.where(strict, jnp.einsum('...id,...jd->...ij', scaled, unit_keys, precision=exact_mode) * within, 0.0)
    inverse = nilpotent_inverse(mixing)
    writes = jnp.einsum('...ij,...je->...ie', inverse, values * strength[..., None], precision=exact_mode)
    erases = jnp.einsum('...ij,...jd->...id', inverse, scaled * jnp.exp(running)[..., None], precision=exact_mode)
    final_log = running[..., -1]
    carried = unit_keys * jnp.exp(final_log[..., None] - running)[..., None]
    return (writes, erases, carried, final_log)

def split_blocks(array, block_count):
    shaped = array.reshape(array.shape[:2] + (block_count, array.shape[2] // block_count) + array.shape[3:])
    return jnp.moveaxis(shaped, 2, 0)

def reference(tokens, key_matrix, value_matrix, gate_matrix, head_decay_rate, extra_log_decay, next_token_query, next_token_key, next_token_value, next_write_strength, read_norm_gain):
    key_proj = jnp.dot(tokens, key_matrix, preferred_element_type=jnp.float32).astype(jnp.bfloat16)
    value_proj = jnp.dot(tokens, value_matrix, preferred_element_type=jnp.float32).astype(jnp.bfloat16)
    gate_pre = jnp.dot(tokens, gate_matrix, preferred_element_type=jnp.float32)
    key_float = lax.optimization_barrier(key_proj).astype(jnp.float32)
    value_float = lax.optimization_barrier(value_proj).astype(jnp.float32)
    unit_keys = unit_rows(key_float.reshape(PROMPT_COUNT, PROMPT_LENGTH, HEAD_COUNT, DK).transpose(0, 2, 1, 3))
    values = value_float.reshape(PROMPT_COUNT, PROMPT_LENGTH, HEAD_COUNT, DV).transpose(0, 2, 1, 3)
    gate_projected = gate_pre.transpose(0, 2, 1)
    decay_logarithm = -head_decay_rate[None, :, None] * jax.nn.softplus(gate_projected[:, :HEAD_COUNT]) + extra_log_decay
    strength = jax.nn.sigmoid(gate_projected[:, HEAD_COUNT:] - strength_offset)
    block_count = PROMPT_LENGTH // BLOCK
    block_parts = block_terms(split_blocks(unit_keys, block_count), split_blocks(values, block_count), split_blocks(decay_logarithm, block_count), split_blocks(strength, block_count))

    def advance(current, block_part):
        writes, erases, carried, final_log = block_part
        fresh = writes - jnp.einsum('shcd,shde->shce', erases, current, precision=exact_mode)
        current = current * jnp.exp(final_log)[..., None, None] + jnp.einsum('shcd,shce->shde', carried, fresh, precision=exact_mode)
        return (current, None)
    start_state = jnp.zeros((PROMPT_COUNT, HEAD_COUNT, DK, DV), jnp.float32)
    state, _ = lax.scan(advance, start_state, block_parts)
    query_rows = next_token_query.astype(jnp.float32).reshape(PROMPT_COUNT, HEAD_COUNT, DK)
    unit_new = unit_rows(next_token_key.astype(jnp.float32).reshape(PROMPT_COUNT, HEAD_COUNT, DK))
    value_rows = next_token_value.astype(jnp.float32)
    key_read = jnp.einsum('shd,shde->she', unit_new, state, precision=exact_mode)
    query_read = jnp.einsum('shd,shde->she', query_rows, state, precision=exact_mode)
    intersection = lax.optimization_barrier(jnp.sum(query_rows * unit_new, axis=-1))
    read_raw = query_read + (next_write_strength * intersection)[..., None] * (value_rows - key_read)
    first_read = read_raw * lax.rsqrt(lax.optimization_barrier(jnp.mean(read_raw * read_raw, axis=-1, keepdims=True)) + 1e-06) * read_norm_gain
    return (state.astype(jnp.bfloat16), first_read.astype(jnp.bfloat16))
```

```python
import functools

import jax
import jax.numpy as jnp
from jax import lax
from jax.experimental import pallas as pl
from jax.experimental.pallas import tpu as pltpu
from jax.sharding import PartitionSpec as P

DV = 128
CORES = 2
MESH = pl.DeviceIdType.MESH


exact_mode = lax.Precision.HIGHEST
strength_offset = 5.0


def unit_rows(matrix):
    return matrix * lax.rsqrt(jnp.sum(matrix * matrix, axis=-1, keepdims=True) + 1e-06)


def nilpotent_inverse(mixing):
    extent = mixing.shape[-1]
    result = jnp.zeros_like(mixing) + jnp.eye(extent, dtype=jnp.float32)
    powered = -mixing
    covered = 1
    while covered < extent:
        product = lax.optimization_barrier(
            jnp.einsum("...ij,...jk->...ik", result, powered, precision=exact_mode)
        )
        result = result + product
        powered = jnp.einsum("...ij,...jk->...ik", powered, powered, precision=exact_mode)
        covered = covered * 2
    return result


def block_terms(unit_keys, values, decay_logarithm, strength):
    extent = unit_keys.shape[-2]
    lower = jnp.tril(jnp.ones((extent, extent), jnp.bool_))
    strict = jnp.tril(jnp.ones((extent, extent), jnp.bool_), -1)
    running = jnp.cumsum(decay_logarithm, axis=-1)
    spread = running[..., :, None] - running[..., None, :]
    within = jnp.where(lower, jnp.exp(jnp.where(lower, spread, 0.0)), 0.0)
    scaled = unit_keys * strength[..., None]
    mixing = jnp.where(
        strict,
        jnp.einsum("...id,...jd->...ij", scaled, unit_keys, precision=exact_mode) * within,
        0.0,
    )
    inverse = nilpotent_inverse(mixing)
    writes = jnp.einsum(
        "...ij,...je->...ie", inverse, values * strength[..., None], precision=exact_mode
    )
    erases = jnp.einsum(
        "...ij,...jd->...id", inverse, scaled * jnp.exp(running)[..., None], precision=exact_mode
    )
    final_log = running[..., -1]
    carried = unit_keys * jnp.exp(final_log[..., None] - running)[..., None]
    return (writes, erases, carried, final_log)


def split_blocks(array, block_count):
    shaped = array.reshape(
        array.shape[:2] + (block_count, array.shape[2] // block_count) + array.shape[3:]
    )
    return jnp.moveaxis(shaped, 2, 0)


def local_general(
    tokens,
    key_matrix,
    value_matrix,
    gate_matrix,
    head_decay_rate,
    extra_log_decay,
    next_token_query,
    next_token_key,
    next_token_value,
    next_write_strength,
    read_norm_gain,
):
    sequences, positions, _ = tokens.shape
    local_heads = head_decay_rate.shape[0]
    key_width = key_matrix.shape[1] // local_heads
    value_width = value_matrix.shape[1] // local_heads
    all_heads = gate_matrix.shape[1] // 2
    group_size = lax.axis_size("sp")
    column_share = value_width // group_size
    first_head = lax.axis_index("tp") * local_heads
    decay_cols = lax.dynamic_slice_in_dim(gate_matrix, first_head, local_heads, 1)
    strength_cols = lax.dynamic_slice_in_dim(gate_matrix, all_heads + first_head, local_heads, 1)
    gate_cols = jnp.concatenate([decay_cols, strength_cols], axis=1)
    row_count = sequences * positions
    incoming = lax.all_gather(tokens, "tp", axis=2, tiled=True)
    span_width = incoming.shape[2]
    flat_rows = incoming.reshape(row_count, span_width)
    products = lax.optimization_barrier(
        (
            jnp.dot(flat_rows, key_matrix, preferred_element_type=jnp.float32),
            jnp.dot(flat_rows, value_matrix, preferred_element_type=jnp.float32),
            jnp.dot(flat_rows, gate_cols, preferred_element_type=jnp.float32),
        )
    )
    key_sum = products[0]
    value_sum = products[1]
    gate_pre = products[2]
    key_float = lax.optimization_barrier(key_sum.astype(jnp.bfloat16)).astype(jnp.float32)
    value_float = lax.optimization_barrier(value_sum.astype(jnp.bfloat16)).astype(jnp.float32)
    unit_keys = unit_rows(
        key_float.reshape(sequences, positions, local_heads, key_width).transpose(0, 2, 1, 3)
    )
    values = value_float.reshape(sequences, positions, local_heads, value_width).transpose(
        0, 2, 1, 3
    )
    gate_projected = gate_pre.reshape(sequences, positions, 2 * local_heads).transpose(0, 2, 1)
    decay_logarithm = (
        -head_decay_rate[None, :, None] * jax.nn.softplus(gate_projected[:, :local_heads])
        + extra_log_decay
    )
    strength = jax.nn.sigmoid(gate_projected[:, local_heads:] - strength_offset)
    block_count = positions // min(64, positions)
    block_parts = block_terms(
        split_blocks(unit_keys, block_count),
        split_blocks(values, block_count),
        split_blocks(decay_logarithm, block_count),
        split_blocks(strength, block_count),
    )
    identity = jnp.zeros((sequences, local_heads, key_width, key_width), jnp.float32) + jnp.eye(
        key_width, dtype=jnp.float32
    )
    start_map = jnp.concatenate(
        [identity, jnp.zeros((sequences, local_heads, key_width, value_width), jnp.float32)],
        axis=-1,
    )

    def advance(current, block_part):
        writes, erases, carried, final_log = block_part
        padded = jnp.concatenate(
            [jnp.zeros(writes.shape[:-1] + (key_width,), jnp.float32), writes], axis=-1
        )
        removed = lax.optimization_barrier(
            jnp.einsum("shcd,shde->shce", erases, current, precision=exact_mode)
        )
        fresh = padded - removed
        added = lax.optimization_barrier(
            jnp.einsum("shcd,shce->shde", carried, fresh, precision=exact_mode)
        )
        current = current * jnp.exp(final_log)[..., None, None] + added
        return (current, None)

    local_map, _ = lax.scan(advance, start_map, block_parts)
    carry_map = local_map[..., :key_width]
    write_map = local_map[..., key_width:]
    carry_copies = jnp.broadcast_to(carry_map[None], (group_size,) + carry_map.shape)
    write_parts = jnp.moveaxis(
        write_map.reshape(sequences, local_heads, key_width, group_size, column_share), 3, 0
    )
    carries = lax.all_to_all(carry_copies, "sp", split_axis=0, concat_axis=0, tiled=True)
    write_cols = lax.all_to_all(write_parts, "sp", split_axis=0, concat_axis=0, tiled=True)

    def fold_step(current, block_map):
        moved = lax.optimization_barrier(
            jnp.einsum("shij,shje->shie", block_map[0], current, precision=exact_mode)
        )
        return (moved + block_map[1], None)

    begin_state = jnp.zeros(write_cols.shape[1:], jnp.float32)
    folded, _ = lax.scan(fold_step, begin_state, (carries, write_cols))
    query_rows = next_token_query.astype(jnp.float32).reshape(sequences, local_heads, key_width)
    unit_new = unit_rows(
        next_token_key.astype(jnp.float32).reshape(sequences, local_heads, key_width)
    )
    value_rows = next_token_value.astype(jnp.float32)
    key_read = jnp.einsum("shd,shde->she", unit_new, folded, precision=exact_mode)
    query_read = jnp.einsum("shd,shde->she", query_rows, folded, precision=exact_mode)
    intersection = jnp.sum(query_rows * unit_new, axis=-1)
    read_raw = query_read + (next_write_strength * intersection)[..., None] * (
        value_rows - key_read
    )
    square_total = lax.psum(jnp.sum(read_raw * read_raw, axis=-1, keepdims=True), "sp")
    first_read = read_raw * lax.rsqrt(square_total / DV + 1e-06) * read_norm_gain
    return (folded.astype(jnp.bfloat16), first_read.astype(jnp.bfloat16))


def exact_dot(left, right, contract=((1,), (0,))):
    return lax.dot_general(
        left, right, (contract, ((), ())), precision=exact_mode, preferred_element_type=jnp.float32
    )


def short_dot(left, right, contract=((1,), (0,))):
    return lax.dot_general(
        left.astype(jnp.bfloat16),
        right.astype(jnp.bfloat16),
        (contract, ((), ())),
        preferred_element_type=jnp.float32,
    )


def softplus(x):
    return jnp.maximum(x, 0.0) + jnp.log1p(jnp.exp(-jnp.abs(x)))


def grid_mask(rows, cols, rule):
    row = lax.broadcasted_iota(jnp.int32, (rows, cols), 0)
    col = lax.broadcasted_iota(jnp.int32, (rows, cols), 1)
    return rule(row, col)


def fused_kernel(
    sp_size,
    tp_size,
    rate_ref,
    next_strength_ref,
    tokens_ref,
    key_ref,
    value_ref,
    gate_ref,
    extra_ref,
    query_ref,
    new_key_ref,
    new_value_ref,
    gain_ref,
    state_ref,
    read_ref,
    gathered,
    key_w,
    value_w,
    key_acc,
    value_acc,
    gate_acc,
    kv_out,
    kv_in,
    side_out,
    side_in,
    state_out,
    state_in,
    row_out,
    row_in,
    load_sem,
    weight_sem,
    gather_recv,
    gather_send,
    swap_recv,
    swap_send,
    swap_local,
    last_recv,
    last_send,
    last_local,
):
    sequences, positions, depth = tokens_ref.shape
    local_heads = extra_ref.shape[1]
    key_width = key_acc.shape[1] // local_heads
    value_width = value_acc.shape[1] // local_heads
    share = value_width // sp_size
    all_heads = gate_ref.shape[1] // 2
    chips = tp_size // CORES
    me = lax.axis_index("sp")
    spot = lax.axis_index("tp")
    chip = spot // CORES
    core = spot % CORES
    partner = chip * CORES + (1 - core)

    loads = [
        pltpu.make_async_copy(tokens_ref.at[s], gathered.at[spot, s], load_sem.at[s])
        for s in range(sequences)
    ]
    for load in loads:
        load.start()

    barrier = pltpu.get_barrier_semaphore()
    pl.semaphore_signal(barrier, inc=1, device_id={"tp": partner}, device_id_type=MESH)

    @pl.when(chip > 0)
    def _():
        pl.semaphore_signal(barrier, inc=1, device_id={"tp": spot - CORES}, device_id_type=MESH)

    @pl.when(chip < chips - 1)
    def _():
        pl.semaphore_signal(barrier, inc=1, device_id={"tp": spot + CORES}, device_id_type=MESH)

    for offset in range(1, sp_size):
        pl.semaphore_signal(
            barrier, inc=1, device_id={"sp": (me + offset) % sp_size}, device_id_type=MESH
        )
    weights = [
        pltpu.make_async_copy(key_ref, key_w, weight_sem.at[0]),
        pltpu.make_async_copy(value_ref, value_w, weight_sem.at[1]),
    ]
    for weight in weights:
        weight.start()
    key_acc[...] = jnp.zeros_like(key_acc)
    value_acc[...] = jnp.zeros_like(value_acc)
    gate_acc[...] = jnp.zeros_like(gate_acc)
    for load in loads:
        load.wait()
    near = jnp.where(chip > 0, 1, 0) + jnp.where(chip < chips - 1, 1, 0)
    pl.semaphore_wait(barrier, near + sp_size)

    def piece(origin, s, way, target):
        return pltpu.make_async_remote_copy(
            src_ref=gathered.at[origin, s],
            dst_ref=gathered.at[origin, s],
            send_sem=gather_send.at[origin, s, way],
            recv_sem=gather_recv.at[origin, s],
            device_id={"tp": target},
            device_id_type=MESH,
        )

    def take(block):
        rows = gathered[block].reshape(sequences * positions, depth)
        span = pl.ds(pl.multiple_of(block * depth, depth), depth)
        key_acc[...] += jnp.dot(rows, key_w[span, :], preferred_element_type=jnp.float32)
        value_acc[...] += jnp.dot(rows, value_w[span, :], preferred_element_type=jnp.float32)
        gate_acc[...] += jnp.dot(rows, gate_ref[span, :], preferred_element_type=jnp.float32)

    for s in range(sequences):

        @pl.when(chip < chips - 1)
        def _(s=s):
            piece(spot, s, 0, spot + CORES).start()

        @pl.when(chip > 0)
        def _(s=s):
            piece(spot, s, 1, spot - CORES).start()

        piece(spot, s, 2, partner).start()
    for weight in weights:
        weight.wait()
    take(spot)
    for s in range(sequences):
        piece(partner, s, 2, partner).wait_recv()
    take(partner)

    for distance in range(1, chips):
        for s in range(sequences):
            for way, step in ((0, -1), (1, 1)):
                origin_chip = chip + step * distance
                origin = origin_chip * CORES + core
                present = (origin_chip >= 0) & (origin_chip < chips)
                onward = chip - step

                @pl.when(present)
                def _(s=s, way=way, origin=origin, onward=onward):
                    piece(origin, s, way, partner).wait_recv()

                    @pl.when((onward >= 0) & (onward < chips))
                    def _():
                        piece(origin, s, way, onward * CORES + core).start()

                    piece(origin, s, 2, partner).start()

        def absorb(index, carry, distance=distance):
            side = index // CORES
            which = index % CORES
            origin_chip = chip + (2 * side - 1) * distance
            present = (origin_chip >= 0) & (origin_chip < chips)

            @pl.when(present & (which == 0))
            def _():
                take(origin_chip * CORES + core)

            @pl.when(present & (which == 1))
            def _():
                block = origin_chip * CORES + 1 - core
                for s in range(sequences):
                    piece(block, s, 2, partner).wait_recv()
                take(block)

            return carry

        lax.fori_loop(0, 2 * CORES, absorb, 0)

    first = spot * local_heads
    chooser = grid_mask(
        2 * local_heads,
        2 * all_heads,
        lambda r, c: c == jnp.where(r < local_heads, first + r, all_heads + first + r - local_heads),
    ).astype(jnp.float32)
    gates = exact_dot(chooser, gate_acc[...], ((1,), (1,)))
    placer = grid_mask(share, value_width, lambda r, c: c == me * share + r).astype(jnp.float32)
    side_out[...] = jnp.zeros_like(side_out)
    for s in range(sequences):
        cut = slice(s * positions, (s + 1) * positions)
        new_value = exact_dot(new_value_ref[s].astype(jnp.float32), placer)
        extra = extra_ref[s]
        for h in range(local_heads):
            kv_out[h, 0, s] = key_acc[cut, h * key_width : (h + 1) * key_width].astype(jnp.bfloat16)
            kv_out[h, 1, s] = value_acc[cut, h * value_width : (h + 1) * value_width].astype(
                jnp.bfloat16
            )
            side_out[h, s : s + 1, :] = (
                -rate_ref[h] * softplus(gates[h : h + 1, cut]) + extra[h : h + 1, :]
            )
            side_out[h, 2 + s : 3 + s, :] = jax.nn.sigmoid(
                gates[local_heads + h : local_heads + h + 1, cut] - strength_offset
            )
            side_out[h, 4 + s : 5 + s, :] = new_value[h : h + 1, :]

    def swap(target, origin):
        return [
            pltpu.make_async_remote_copy(
                src_ref=source.at[target],
                dst_ref=sink.at[origin],
                send_sem=swap_send.at[n, target],
                recv_sem=swap_recv.at[n, origin],
                device_id={"sp": target},
                device_id_type=MESH,
            )
            for n, (source, sink) in enumerate(((kv_out, kv_in), (side_out, side_in)))
        ]

    for offset in range(1, sp_size):
        for copy in swap((me + offset) % sp_size, me):
            copy.start()
    kept = [
        pltpu.make_async_copy(kv_out.at[me], kv_in.at[me], swap_local.at[0]),
        pltpu.make_async_copy(side_out.at[me], side_in.at[me], swap_local.at[1]),
    ]
    for copy in kept:
        copy.start()
    for copy in kept:
        copy.wait()
    for offset in range(1, sp_size):
        source = (me + offset) % sp_size
        for n, sink in enumerate((kv_in, side_in)):
            pltpu.make_async_remote_copy(
                src_ref=sink.at[source],
                dst_ref=sink.at[source],
                send_sem=swap_send.at[n, source],
                recv_sem=swap_recv.at[n, source],
                device_id={"sp": source},
                device_id_type=MESH,
            ).wait_recv()

    side_rows = side_in.shape[1]
    side = side_in[...].reshape(sp_size * side_rows, positions)
    upto = grid_mask(positions, positions, lambda r, c: r <= c).astype(jnp.float32)
    eye = grid_mask(positions, positions, lambda r, c: r == c).astype(jnp.float32)
    running_row = exact_dot(side, upto)
    running_col = exact_dot(upto, side, ((0,), (1,)))
    side_col = exact_dot(eye, side, ((1,), (1,)))
    lower = grid_mask(positions, positions, lambda r, c: r >= c)
    strict = grid_mask(positions, positions, lambda r, c: r > c)

    parts = []
    for s in range(sequences):
        for b in range(sp_size):
            line = b * side_rows + s
            row = running_row[line : line + 1, :]
            col = running_col[:, line : line + 1]
            strength = side_col[:, line + 2 : line + 3]
            final_log = row[:, positions - 1 : positions]
            keys = kv_in[b, 0, s].astype(jnp.float32)
            keys = keys * lax.rsqrt(jnp.sum(keys * keys, axis=-1, keepdims=True) + 1e-06)
            within = jnp.where(lower, jnp.exp(jnp.where(lower, col - row, 0.0)), 0.0)
            scaled = keys * strength
            power = jnp.where(strict, -short_dot(scaled, keys, ((1,), (1,))) * within, 0.0)
            targets = jnp.concatenate(
                [kv_in[b, 1, s].astype(jnp.float32) * strength, scaled * jnp.exp(col)], axis=1
            ).astype(jnp.bfloat16)
            carried = (keys * jnp.exp(final_log - col)).T.astype(jnp.bfloat16)
            parts.append([eye + power, power, targets, carried, jnp.exp(final_log)])
    for part in parts:
        part[1] = short_dot(part[1], part[1])
    covered = 2
    while covered < positions:
        for part in parts:
            if covered * 2 < positions:
                both = short_dot(part[1], jnp.concatenate([part[0], part[1]], axis=1))
                part[0] = part[0] + both[:, :positions]
                part[1] = both[:, positions:]
            else:
                part[0] = part[0] + short_dot(part[1], part[0])
        covered = covered * 2
    for part in parts:
        part[2] = short_dot(part[0], part[2])
    states = []
    for s in range(sequences):
        state = None
        for b in range(sp_size):
            _, _, solved, carried, shrink = parts[s * sp_size + b]
            fresh = solved[:, :value_width]
            if state is None:
                state = short_dot(carried, fresh)
            else:
                fresh = fresh - short_dot(solved[:, value_width:], state)
                state = state * shrink + short_dot(carried, fresh)
        states.append(state)

    lanes = pl.ds(pl.multiple_of(me * key_width, key_width), key_width)
    queries = query_ref[:, lanes].astype(jnp.float32)
    new_keys = new_key_ref[:, lanes].astype(jnp.float32)
    new_keys = new_keys * lax.rsqrt(jnp.sum(new_keys * new_keys, axis=-1, keepdims=True) + 1e-06)
    meets = jnp.sum(queries * new_keys, axis=-1, keepdims=True)
    row_out[...] = jnp.zeros_like(row_out)
    for s in range(sequences):
        state = states[s]
        turned = state.T.astype(jnp.bfloat16)
        for j in range(sp_size):
            state_out[j, s] = turned[j * share : (j + 1) * share, :]
        wide = (8, key_width)
        query_read = exact_dot(jnp.broadcast_to(queries[s : s + 1], wide), state)[:1]
        key_read = exact_dot(jnp.broadcast_to(new_keys[s : s + 1], wide), state)[:1]
        new_value = jnp.sum(side_in[:, 4 + s, :], axis=0, keepdims=True)
        raw = query_read + (next_strength_ref[s, me] * meets[s : s + 1]) * (new_value - key_read)
        row_out[s : s + 1, :] = raw * lax.rsqrt(
            jnp.sum(raw * raw, axis=-1, keepdims=True) / value_width + 1e-06
        )

    def final(n, source, sink, target, origin):
        return pltpu.make_async_remote_copy(
            src_ref=source,
            dst_ref=sink.at[origin],
            send_sem=last_send.at[n, target],
            recv_sem=last_recv.at[n, origin],
            device_id={"sp": target},
            device_id_type=MESH,
        )

    for offset in range(1, sp_size):
        target = (me + offset) % sp_size
        final(0, state_out.at[target], state_in, target, me).start()
        final(1, row_out, row_in, target, me).start()
    kept = [
        pltpu.make_async_copy(state_out.at[me], state_in.at[me], last_local.at[0]),
        pltpu.make_async_copy(row_out, row_in.at[me], last_local.at[1]),
    ]
    for copy in kept:
        copy.start()
    for copy in kept:
        copy.wait()
    for offset in range(1, sp_size):
        source = (me + offset) % sp_size
        final(0, state_in.at[source], state_in, source, source).wait_recv()
        final(1, row_in.at[source], row_in, source, source).wait_recv()

    picker = grid_mask(value_width, share, lambda r, c: r == me * share + c).astype(jnp.float32)
    row_lines = row_in.shape[1]
    rows = exact_dot(row_in[...].reshape(sp_size * row_lines, value_width), picker)
    rows = rows * gain_ref[...].reshape(1, share)
    for s in range(sequences):
        read_ref[s] = jnp.concatenate(
            [rows[i * row_lines + s : i * row_lines + s + 1] for i in range(sp_size)], axis=0
        ).astype(jnp.bfloat16)
        for i in range(sp_size):
            state_ref[s, i] = state_in[i, s].astype(jnp.float32).T.astype(jnp.bfloat16)

    for offset in range(1, sp_size):
        target = (me + offset) % sp_size
        for copy in swap(target, me):
            copy.wait_send()
        final(0, state_out.at[target], state_in, target, me).wait_send()
        final(1, row_out, row_in, target, me).wait_send()
    for distance in range(chips):
        for way, step in ((0, -1), (1, 1)):
            if distance == 0 and way == 1:
                continue
            origin_chip = chip + step * distance
            origin = origin_chip * CORES + core

            @pl.when((origin_chip >= 0) & (origin_chip < chips))
            def _(origin=origin):
                for s in range(sequences):
                    piece(origin, s, 2, partner).wait_send()

            for other, onward in ((0, chip + 1), (1, chip - 1)):
                if distance and other != way:
                    continue

                @pl.when(
                    (origin_chip >= 0)
                    & (origin_chip < chips)
                    & (onward >= 0)
                    & (onward < chips)
                )
                def _(origin=origin, other=other, onward=onward):
                    for s in range(sequences):
                        piece(origin, s, other, onward * CORES + core).wait_send()


def local_fused(
    tokens,
    key_matrix,
    value_matrix,
    gate_matrix,
    head_decay_rate,
    extra_log_decay,
    next_token_query,
    next_token_key,
    next_token_value,
    next_write_strength,
    read_norm_gain,
):
    sequences, positions, depth = tokens.shape
    local_heads = head_decay_rate.shape[0]
    sp_size = lax.axis_size("sp")
    tp_size = lax.axis_size("tp")
    key_total = key_matrix.shape[1]
    value_total = value_matrix.shape[1]
    key_width = key_total // local_heads
    value_width = value_total // local_heads
    share = value_width // sp_size
    rows = sequences * positions
    side_rows = 8 * ((3 * sequences + 7) // 8)
    row_lines = 8 * ((sequences + 7) // 8)
    vmem = pl.BlockSpec(memory_space=pltpu.VMEM)
    smem = pl.BlockSpec(memory_space=pltpu.SMEM)
    anywhere = pl.BlockSpec(memory_space=pl.ANY)
    dma = pltpu.SemaphoreType.DMA
    return pl.pallas_call(
        functools.partial(fused_kernel, sp_size, tp_size),
        out_shape=(
            jax.ShapeDtypeStruct((sequences, local_heads, key_width, share), jnp.bfloat16),
            jax.ShapeDtypeStruct((sequences, local_heads, share), jnp.bfloat16),
        ),
        in_specs=[smem, smem, anywhere, anywhere, anywhere] + [vmem] * 6,
        out_specs=(vmem, vmem),
        scratch_shapes=[
            pltpu.VMEM((tp_size, sequences, positions, depth), jnp.bfloat16),
            pltpu.VMEM(key_matrix.shape, jnp.bfloat16),
            pltpu.VMEM(value_matrix.shape, jnp.bfloat16),
            pltpu.VMEM((rows, key_total), jnp.float32),
            pltpu.VMEM((rows, value_total), jnp.float32),
            pltpu.VMEM((rows, gate_matrix.shape[1]), jnp.float32),
            pltpu.VMEM((sp_size, 2, sequences, positions, key_width), jnp.bfloat16),
            pltpu.VMEM((sp_size, 2, sequences, positions, key_width), jnp.bfloat16),
            pltpu.VMEM((sp_size, side_rows, positions), jnp.float32),
            pltpu.VMEM((sp_size, side_rows, positions), jnp.float32),
            pltpu.VMEM((sp_size, sequences, share, key_width), jnp.bfloat16),
            pltpu.VMEM((sp_size, sequences, share, key_width), jnp.bfloat16),
            pltpu.VMEM((row_lines, value_width), jnp.float32),
            pltpu.VMEM((sp_size, row_lines, value_width), jnp.float32),
            dma((sequences,)),
            dma((2,)),
            dma((tp_size, sequences)),
            dma((tp_size, sequences, 3)),
            dma((2, sp_size)),
            dma((2, sp_size)),
            dma((2,)),
            dma((2, sp_size)),
            dma((2, sp_size)),
            dma((2,)),
        ],
        compiler_params=pltpu.CompilerParams(
            collective_id=0, has_side_effects=True, vmem_limit_bytes=48 * 1024 * 1024
        ),
    )(
        head_decay_rate,
        next_write_strength,
        tokens,
        key_matrix,
        value_matrix,
        gate_matrix,
        extra_log_decay,
        next_token_query,
        next_token_key,
        next_token_value,
        read_norm_gain,
    )


def local(*arguments):
    tokens, key_matrix, value_matrix = arguments[:3]
    sequences, positions, _ = tokens.shape
    local_heads = arguments[4].shape[0]
    sp_size = lax.axis_size("sp")
    fits = (
        local_heads == sp_size
        and sequences == 2
        and lax.axis_size("tp") % CORES == 0
        and positions == key_matrix.shape[1] // local_heads
        and positions == value_matrix.shape[1] // local_heads
        and positions % 128 == 0
    )
    return local_fused(*arguments) if fits else local_general(*arguments)


def solution(mesh):
    in_specs = (
        P(None, "sp", "tp"),
        P(None, "tp"),
        P(None, "tp"),
        P(),
        P("tp"),
        P(None, "tp", "sp"),
        P(None, "tp"),
        P(None, "tp"),
        P(None, "tp", "sp"),
        P(None, "tp"),
        P("sp"),
    )
    out_specs = (P(None, "tp", None, "sp"), P(None, "tp", "sp"))
    return jax.shard_map(local, mesh=mesh, in_specs=in_specs, out_specs=out_specs, check_vma=False)
```

```python
import functools

import jax
import jax.numpy as jnp
from jax import lax
from jax.experimental import pallas as pl
from jax.experimental.pallas import tpu as pltpu
from jax.sharding import PartitionSpec as P

DV = 128
CORES = 2
MESH = pl.DeviceIdType.MESH


exact_mode = lax.Precision.HIGHEST
strength_offset = 5.0


def unit_rows(matrix):
    return matrix * lax.rsqrt(jnp.sum(matrix * matrix, axis=-1, keepdims=True) + 1e-06)


def nilpotent_inverse(mixing):
    extent = mixing.shape[-1]
    result = jnp.zeros_like(mixing) + jnp.eye(extent, dtype=jnp.float32)
    powered = -mixing
    covered = 1
    while covered < extent:
        product = lax.optimization_barrier(
            jnp.einsum("...ij,...jk->...ik", result, powered, precision=exact_mode)
        )
        result = result + product
        powered = jnp.einsum("...ij,...jk->...ik", powered, powered, precision=exact_mode)
        covered = covered * 2
    return result


def block_terms(unit_keys, values, decay_logarithm, strength):
    extent = unit_keys.shape[-2]
    lower = jnp.tril(jnp.ones((extent, extent), jnp.bool_))
    strict = jnp.tril(jnp.ones((extent, extent), jnp.bool_), -1)
    running = jnp.cumsum(decay_logarithm, axis=-1)
    spread = running[..., :, None] - running[..., None, :]
    within = jnp.where(lower, jnp.exp(jnp.where(lower, spread, 0.0)), 0.0)
    scaled = unit_keys * strength[..., None]
    mixing = jnp.where(
        strict,
        jnp.einsum("...id,...jd->...ij", scaled, unit_keys, precision=exact_mode) * within,
        0.0,
    )
    inverse = nilpotent_inverse(mixing)
    writes = jnp.einsum(
        "...ij,...je->...ie", inverse, values * strength[..., None], precision=exact_mode
    )
    erases = jnp.einsum(
        "...ij,...jd->...id", inverse, scaled * jnp.exp(running)[..., None], precision=exact_mode
    )
    final_log = running[..., -1]
    carried = unit_keys * jnp.exp(final_log[..., None] - running)[..., None]
    return (writes, erases, carried, final_log)


def split_blocks(array, block_count):
    shaped = array.reshape(
        array.shape[:2] + (block_count, array.shape[2] // block_count) + array.shape[3:]
    )
    return jnp.moveaxis(shaped, 2, 0)


def local_general(
    tokens,
    key_matrix,
    value_matrix,
    gate_matrix,
    head_decay_rate,
    extra_log_decay,
    next_token_query,
    next_token_key,
    next_token_value,
    next_write_strength,
    read_norm_gain,
):
    sequences, positions, _ = tokens.shape
    local_heads = head_decay_rate.shape[0]
    key_width = key_matrix.shape[1] // local_heads
    value_width = value_matrix.shape[1] // local_heads
    all_heads = gate_matrix.shape[1] // 2
    group_size = lax.axis_size("sp")
    column_share = value_width // group_size
    first_head = lax.axis_index("tp") * local_heads
    decay_cols = lax.dynamic_slice_in_dim(gate_matrix, first_head, local_heads, 1)
    strength_cols = lax.dynamic_slice_in_dim(gate_matrix, all_heads + first_head, local_heads, 1)
    gate_cols = jnp.concatenate([decay_cols, strength_cols], axis=1)
    row_count = sequences * positions
    incoming = lax.all_gather(tokens, "tp", axis=2, tiled=True)
    span_width = incoming.shape[2]
    flat_rows = incoming.reshape(row_count, span_width)
    products = lax.optimization_barrier(
        (
            jnp.dot(flat_rows, key_matrix, preferred_element_type=jnp.float32),
            jnp.dot(flat_rows, value_matrix, preferred_element_type=jnp.float32),
            jnp.dot(flat_rows, gate_cols, preferred_element_type=jnp.float32),
        )
    )
    key_sum = products[0]
    value_sum = products[1]
    gate_pre = products[2]
    key_float = lax.optimization_barrier(key_sum.astype(jnp.bfloat16)).astype(jnp.float32)
    value_float = lax.optimization_barrier(value_sum.astype(jnp.bfloat16)).astype(jnp.float32)
    unit_keys = unit_rows(
        key_float.reshape(sequences, positions, local_heads, key_width).transpose(0, 2, 1, 3)
    )
    values = value_float.reshape(sequences, positions, local_heads, value_width).transpose(
        0, 2, 1, 3
    )
    gate_projected = gate_pre.reshape(sequences, positions, 2 * local_heads).transpose(0, 2, 1)
    decay_logarithm = (
        -head_decay_rate[None, :, None] * jax.nn.softplus(gate_projected[:, :local_heads])
        + extra_log_decay
    )
    strength = jax.nn.sigmoid(gate_projected[:, local_heads:] - strength_offset)
    block_count = positions // min(64, positions)
    block_parts = block_terms(
        split_blocks(unit_keys, block_count),
        split_blocks(values, block_count),
        split_blocks(decay_logarithm, block_count),
        split_blocks(strength, block_count),
    )
    identity = jnp.zeros((sequences, local_heads, key_width, key_width), jnp.float32) + jnp.eye(
        key_width, dtype=jnp.float32
    )
    start_map = jnp.concatenate(
        [identity, jnp.zeros((sequences, local_heads, key_width, value_width), jnp.float32)],
        axis=-1,
    )

    def advance(current, block_part):
        writes, erases, carried, final_log = block_part
        padded = jnp.concatenate(
            [jnp.zeros(writes.shape[:-1] + (key_width,), jnp.float32), writes], axis=-1
        )
        removed = lax.optimization_barrier(
            jnp.einsum("shcd,shde->shce", erases, current, precision=exact_mode)
        )
        fresh = padded - removed
        added = lax.optimization_barrier(
            jnp.einsum("shcd,shce->shde", carried, fresh, precision=exact_mode)
        )
        current = current * jnp.exp(final_log)[..., None, None] + added
        return (current, None)

    local_map, _ = lax.scan(advance, start_map, block_parts)
    carry_map = local_map[..., :key_width]
    write_map = local_map[..., key_width:]
    carry_copies = jnp.broadcast_to(carry_map[None], (group_size,) + carry_map.shape)
    write_parts = jnp.moveaxis(
        write_map.reshape(sequences, local_heads, key_width, group_size, column_share), 3, 0
    )
    carries = lax.all_to_all(carry_copies, "sp", split_axis=0, concat_axis=0, tiled=True)
    write_cols = lax.all_to_all(write_parts, "sp", split_axis=0, concat_axis=0, tiled=True)

    def fold_step(current, block_map):
        moved = lax.optimization_barrier(
            jnp.einsum("shij,shje->shie", block_map[0], current, precision=exact_mode)
        )
        return (moved + block_map[1], None)

    begin_state = jnp.zeros(write_cols.shape[1:], jnp.float32)
    folded, _ = lax.scan(fold_step, begin_state, (carries, write_cols))
    query_rows = next_token_query.astype(jnp.float32).reshape(sequences, local_heads, key_width)
    unit_new = unit_rows(
        next_token_key.astype(jnp.float32).reshape(sequences, local_heads, key_width)
    )
    value_rows = next_token_value.astype(jnp.float32)
    key_read = jnp.einsum("shd,shde->she", unit_new, folded, precision=exact_mode)
    query_read = jnp.einsum("shd,shde->she", query_rows, folded, precision=exact_mode)
    intersection = jnp.sum(query_rows * unit_new, axis=-1)
    read_raw = query_read + (next_write_strength * intersection)[..., None] * (
        value_rows - key_read
    )
    square_total = lax.psum(jnp.sum(read_raw * read_raw, axis=-1, keepdims=True), "sp")
    first_read = read_raw * lax.rsqrt(square_total / DV + 1e-06) * read_norm_gain
    return (folded.astype(jnp.bfloat16), first_read.astype(jnp.bfloat16))


def exact_dot(left, right, contract=((1,), (0,))):
    return lax.dot_general(
        left, right, (contract, ((), ())), precision=exact_mode, preferred_element_type=jnp.float32
    )


def short_dot(left, right, contract=((1,), (0,))):
    return lax.dot_general(
        left.astype(jnp.bfloat16),
        right.astype(jnp.bfloat16),
        (contract, ((), ())),
        preferred_element_type=jnp.float32,
    )


def softplus(x):
    return jnp.maximum(x, 0.0) + jnp.log1p(jnp.exp(-jnp.abs(x)))


def grid_mask(rows, cols, rule):
    row = lax.broadcasted_iota(jnp.int32, (rows, cols), 0)
    col = lax.broadcasted_iota(jnp.int32, (rows, cols), 1)
    return rule(row, col)


def fused_kernel(
    sp_size,
    tp_size,
    rate_ref,
    next_strength_ref,
    tokens_ref,
    key_ref,
    value_ref,
    gate_hbm,
    extra_hbm,
    query_hbm,
    new_key_hbm,
    new_value_hbm,
    gain_hbm,
    state_ref,
    read_ref,
    gathered,
    key_w,
    value_w,
    gate_ref,
    extra_ref,
    query_ref,
    new_key_ref,
    new_value_ref,
    gain_ref,
    key_acc,
    value_acc,
    gate_acc,
    kv_out,
    kv_in,
    side_out,
    side_in,
    state_out,
    state_in,
    row_out,
    row_in,
    load_sem,
    weight_sem,
    gather_recv,
    gather_send,
    swap_recv,
    swap_send,
    swap_local,
    last_recv,
    last_send,
    last_local,
):
    sequences, positions, depth = tokens_ref.shape
    local_heads = extra_ref.shape[1]
    key_width = key_acc.shape[1] // local_heads
    value_width = value_acc.shape[1] // local_heads
    share = value_width // sp_size
    all_heads = gate_ref.shape[0] // 2
    chips = tp_size // CORES
    me = lax.axis_index("sp")
    spot = lax.axis_index("tp")
    chip = spot // CORES
    core = spot % CORES
    partner = chip * CORES + (1 - core)

    loads = [
        pltpu.make_async_copy(tokens_ref.at[s], gathered.at[spot, s], load_sem.at[s])
        for s in range(sequences)
    ]
    for load in loads:
        load.start()

    barrier = pltpu.get_barrier_semaphore()
    pl.semaphore_signal(barrier, inc=1, device_id={"tp": partner}, device_id_type=MESH)

    @pl.when(chip > 0)
    def _():
        pl.semaphore_signal(barrier, inc=1, device_id={"tp": spot - CORES}, device_id_type=MESH)

    @pl.when(chip < chips - 1)
    def _():
        pl.semaphore_signal(barrier, inc=1, device_id={"tp": spot + CORES}, device_id_type=MESH)

    for offset in range(1, sp_size):
        pl.semaphore_signal(
            barrier, inc=1, device_id={"sp": (me + offset) % sp_size}, device_id_type=MESH
        )
    weights = [
        pltpu.make_async_copy(key_ref, key_w, weight_sem.at[0]),
        pltpu.make_async_copy(value_ref, value_w, weight_sem.at[1]),
        pltpu.make_async_copy(gate_hbm, gate_ref, weight_sem.at[2]),
        pltpu.make_async_copy(extra_hbm, extra_ref, weight_sem.at[3]),
        pltpu.make_async_copy(query_hbm, query_ref, weight_sem.at[4]),
        pltpu.make_async_copy(new_key_hbm, new_key_ref, weight_sem.at[5]),
        pltpu.make_async_copy(new_value_hbm, new_value_ref, weight_sem.at[6]),
        pltpu.make_async_copy(gain_hbm, gain_ref, weight_sem.at[7]),
    ]
    for weight in weights:
        weight.start()
    key_acc[...] = jnp.zeros_like(key_acc)
    value_acc[...] = jnp.zeros_like(value_acc)
    gate_acc[...] = jnp.zeros_like(gate_acc)
    side_out[...] = jnp.zeros_like(side_out)
    row_out[...] = jnp.zeros_like(row_out)
    for load in loads:
        load.wait()
    near = jnp.where(chip > 0, 1, 0) + jnp.where(chip < chips - 1, 1, 0)
    pl.semaphore_wait(barrier, near + sp_size)

    def piece(origin, s, way, target):
        return pltpu.make_async_remote_copy(
            src_ref=gathered.at[origin, s],
            dst_ref=gathered.at[origin, s],
            send_sem=gather_send.at[origin, s, way],
            recv_sem=gather_recv.at[origin, s],
            device_id={"tp": target},
            device_id_type=MESH,
        )

    def take(block, s):
        rows = gathered[block, s]
        cut = slice(s * positions, (s + 1) * positions)
        span = pl.ds(pl.multiple_of(block * depth, depth), depth)
        key_acc[cut] += jnp.dot(rows, key_w[span, :], preferred_element_type=jnp.float32)
        value_acc[cut] += jnp.dot(rows, value_w[span, :], preferred_element_type=jnp.float32)
        gate_acc[cut] += lax.dot_general(
            rows,
            gate_ref[:, span],
            (((1,), (1,)), ((), ())),
            preferred_element_type=jnp.float32,
        )

    first = spot * local_heads
    chooser = grid_mask(
        2 * local_heads,
        2 * all_heads,
        lambda r, c: c == jnp.where(r < local_heads, first + r, all_heads + first + r - local_heads),
    ).astype(jnp.float32)
    placer = grid_mask(share, value_width, lambda r, c: c == me * share + r).astype(jnp.float32)

    def swap(s, target, origin):
        return [
            pltpu.make_async_remote_copy(
                src_ref=source.at[target, s],
                dst_ref=sink.at[origin, s],
                send_sem=swap_send.at[n, s, target],
                recv_sem=swap_recv.at[n, s, origin],
                device_id={"sp": target},
                device_id_type=MESH,
            )
            for n, (source, sink) in enumerate(((kv_out, kv_in), (side_out, side_in)))
        ]

    def kept(s):
        return [
            pltpu.make_async_copy(kv_out.at[me, s], kv_in.at[me, s], swap_local.at[0, s]),
            pltpu.make_async_copy(side_out.at[me, s], side_in.at[me, s], swap_local.at[1, s]),
        ]

    def hand_out(s):
        cut = slice(s * positions, (s + 1) * positions)
        gates = exact_dot(chooser, gate_acc[cut], ((1,), (1,)))
        new_value = exact_dot(new_value_ref[s].astype(jnp.float32), placer)
        extra = extra_ref[s]
        for h in range(local_heads):
            kv_out[h, s, 0] = key_acc[cut, h * key_width : (h + 1) * key_width].astype(jnp.bfloat16)
            kv_out[h, s, 1] = value_acc[cut, h * value_width : (h + 1) * value_width].astype(
                jnp.bfloat16
            )
            side_out[h, s, 0:1, :] = (
                -rate_ref[h] * softplus(gates[h : h + 1]) + extra[h : h + 1, :]
            )
            side_out[h, s, 1:2, :] = jax.nn.sigmoid(
                gates[local_heads + h : local_heads + h + 1] - strength_offset
            )
            side_out[h, s, 2:3, :] = new_value[h : h + 1, :]
        for offset in range(1, sp_size):
            for copy in swap(s, (me + offset) % sp_size, me):
                copy.start()
        for copy in kept(s):
            copy.start()

    for s in range(sequences):

        @pl.when(chip < chips - 1)
        def _(s=s):
            piece(spot, s, 0, spot + CORES).start()

        @pl.when(chip > 0)
        def _(s=s):
            piece(spot, s, 1, spot - CORES).start()

        piece(spot, s, 2, partner).start()
    for weight in weights:
        weight.wait()
    for s in range(sequences):
        take(spot, s)
        piece(partner, s, 2, partner).wait_recv()
        take(partner, s)

    for distance in range(1, chips):
        for s in range(sequences):
            for way, step in ((0, -1), (1, 1)):
                origin_chip = chip + step * distance
                origin = origin_chip * CORES + core
                present = (origin_chip >= 0) & (origin_chip < chips)
                onward = chip - step

                @pl.when(present)
                def _(s=s, way=way, origin=origin, onward=onward):
                    piece(origin, s, way, partner).wait_recv()

                    @pl.when((onward >= 0) & (onward < chips))
                    def _():
                        piece(origin, s, way, onward * CORES + core).start()

                    piece(origin, s, 2, partner).start()

            def absorb(index, carry, distance=distance, s=s):
                side = index // CORES
                which = index % CORES
                origin_chip = chip + (2 * side - 1) * distance
                present = (origin_chip >= 0) & (origin_chip < chips)

                @pl.when(present & (which == 0))
                def _():
                    take(origin_chip * CORES + core, s)

                @pl.when(present & (which == 1))
                def _():
                    block = origin_chip * CORES + 1 - core
                    piece(block, s, 2, partner).wait_recv()
                    take(block, s)

                return carry

            lax.fori_loop(0, 2 * CORES, absorb, 0)
            if distance == chips - 1:
                hand_out(s)

    side_rows = side_in.shape[2]
    upto = grid_mask(positions, positions, lambda r, c: r <= c).astype(jnp.float32)
    eye = grid_mask(positions, positions, lambda r, c: r == c).astype(jnp.float32)
    lower = grid_mask(positions, positions, lambda r, c: r >= c)
    strict = grid_mask(positions, positions, lambda r, c: r > c)
    lanes = pl.ds(pl.multiple_of(me * key_width, key_width), key_width)
    queries = query_ref[:, lanes].astype(jnp.float32)
    new_keys = new_key_ref[:, lanes].astype(jnp.float32)
    new_keys = new_keys * lax.rsqrt(jnp.sum(new_keys * new_keys, axis=-1, keepdims=True) + 1e-06)
    meets = jnp.sum(queries * new_keys, axis=-1, keepdims=True)

    def final(n, s, source, sink, target, origin):
        return pltpu.make_async_remote_copy(
            src_ref=source,
            dst_ref=sink.at[origin, s],
            send_sem=last_send.at[n, s, target],
            recv_sem=last_recv.at[n, s, origin],
            device_id={"sp": target},
            device_id_type=MESH,
        )

    def stay(s):
        return [
            pltpu.make_async_copy(state_out.at[me, s], state_in.at[me, s], last_local.at[0, s]),
            pltpu.make_async_copy(row_out.at[s], row_in.at[me, s], last_local.at[1, s]),
        ]

    for s in range(sequences):
        for copy in kept(s):
            copy.wait()
        for offset in range(1, sp_size):
            source = (me + offset) % sp_size
            for copy in swap(s, source, source):
                copy.wait_recv()
        side = side_in[:, s].reshape(sp_size * side_rows, positions)
        running_row = exact_dot(side, upto)
        running_col = exact_dot(upto, side, ((0,), (1,)))
        side_col = exact_dot(eye, side, ((1,), (1,)))
        parts = []
        for b in range(sp_size):
            line = b * side_rows
            row = running_row[line : line + 1, :]
            col = running_col[:, line : line + 1]
            strength = side_col[:, line + 1 : line + 2]
            final_log = row[:, positions - 1 : positions]
            keys = kv_in[b, s, 0].astype(jnp.float32)
            keys = keys * lax.rsqrt(jnp.sum(keys * keys, axis=-1, keepdims=True) + 1e-06)
            within = jnp.where(lower, jnp.exp(jnp.where(lower, col - row, 0.0)), 0.0)
            scaled = keys * strength
            power = jnp.where(strict, -short_dot(scaled, keys, ((1,), (1,))) * within, 0.0)
            targets = jnp.concatenate(
                [kv_in[b, s, 1].astype(jnp.float32) * strength, scaled * jnp.exp(col)], axis=1
            ).astype(jnp.bfloat16)
            carried = (keys * jnp.exp(final_log - col)).T.astype(jnp.bfloat16)
            parts.append([eye + power, power, targets, carried, jnp.exp(final_log)])
        for part in parts:
            part[1] = short_dot(part[1], part[1])
        covered = 2
        while covered < positions:
            for part in parts:
                if covered * 2 < positions:
                    both = short_dot(part[1], jnp.concatenate([part[0], part[1]], axis=1))
                    part[0] = part[0] + both[:, :positions]
                    part[1] = both[:, positions:]
                else:
                    part[0] = part[0] + short_dot(part[1], part[0])
            covered = covered * 2
        for part in parts:
            part[2] = short_dot(part[0], part[2])
        state = None
        for _, _, solved, carried, shrink in parts:
            fresh = solved[:, :value_width]
            if state is None:
                state = short_dot(carried, fresh)
            else:
                fresh = fresh - short_dot(solved[:, value_width:], state)
                state = state * shrink + short_dot(carried, fresh)

        turned = state.T.astype(jnp.bfloat16)
        for j in range(sp_size):
            state_out[j, s] = turned[j * share : (j + 1) * share, :]
        for offset in range(1, sp_size):
            target = (me + offset) % sp_size
            final(0, s, state_out.at[target, s], state_in, target, me).start()
        wide = (8, key_width)
        query_read = exact_dot(jnp.broadcast_to(queries[s : s + 1], wide), state)[:1]
        key_read = exact_dot(jnp.broadcast_to(new_keys[s : s + 1], wide), state)[:1]
        new_value = jnp.sum(side_in[:, s, 2, :], axis=0, keepdims=True)
        raw = query_read + (next_strength_ref[s, me] * meets[s : s + 1]) * (new_value - key_read)
        row_out[s, 0:1, :] = raw * lax.rsqrt(
            jnp.sum(raw * raw, axis=-1, keepdims=True) / value_width + 1e-06
        )
        for offset in range(1, sp_size):
            target = (me + offset) % sp_size
            final(1, s, row_out.at[s], row_in, target, me).start()
        for copy in stay(s):
            copy.start()

    picker = grid_mask(value_width, share, lambda r, c: r == me * share + c).astype(jnp.float32)
    row_lines = row_in.shape[2]
    for s in range(sequences):
        for copy in stay(s):
            copy.wait()
        for offset in range(1, sp_size):
            source = (me + offset) % sp_size
            final(0, s, state_in.at[source, s], state_in, source, source).wait_recv()
            final(1, s, row_in.at[source, s], row_in, source, source).wait_recv()
        rows = exact_dot(row_in[:, s].reshape(sp_size * row_lines, value_width), picker)
        rows = rows * gain_ref[...].reshape(1, share)
        read_ref[s] = jnp.concatenate(
            [rows[i * row_lines : i * row_lines + 1] for i in range(sp_size)], axis=0
        ).astype(jnp.bfloat16)
        for i in range(sp_size):
            state_ref[s, i] = state_in[i, s]

    for s in range(sequences):
        for offset in range(1, sp_size):
            target = (me + offset) % sp_size
            for copy in swap(s, target, me):
                copy.wait_send()
            final(0, s, state_out.at[target, s], state_in, target, me).wait_send()
            final(1, s, row_out.at[s], row_in, target, me).wait_send()
    for distance in range(chips):
        for way, step in ((0, -1), (1, 1)):
            if distance == 0 and way == 1:
                continue
            origin_chip = chip + step * distance
            origin = origin_chip * CORES + core

            @pl.when((origin_chip >= 0) & (origin_chip < chips))
            def _(origin=origin):
                for s in range(sequences):
                    piece(origin, s, 2, partner).wait_send()

            for other, onward in ((0, chip + 1), (1, chip - 1)):
                if distance and other != way:
                    continue

                @pl.when(
                    (origin_chip >= 0)
                    & (origin_chip < chips)
                    & (onward >= 0)
                    & (onward < chips)
                )
                def _(origin=origin, other=other, onward=onward):
                    for s in range(sequences):
                        piece(origin, s, other, onward * CORES + core).wait_send()


def local_fused(
    tokens,
    key_matrix,
    value_matrix,
    gate_matrix,
    head_decay_rate,
    extra_log_decay,
    next_token_query,
    next_token_key,
    next_token_value,
    next_write_strength,
    read_norm_gain,
):
    sequences, positions, depth = tokens.shape
    local_heads = head_decay_rate.shape[0]
    sp_size = lax.axis_size("sp")
    tp_size = lax.axis_size("tp")
    key_total = key_matrix.shape[1]
    value_total = value_matrix.shape[1]
    key_width = key_total // local_heads
    value_width = value_total // local_heads
    share = value_width // sp_size
    rows = sequences * positions
    vmem = pl.BlockSpec(memory_space=pltpu.VMEM)
    smem = pl.BlockSpec(memory_space=pltpu.SMEM)
    anywhere = pl.BlockSpec(memory_space=pl.ANY)
    dma = pltpu.SemaphoreType.DMA
    turned, read = pl.pallas_call(
        functools.partial(fused_kernel, sp_size, tp_size),
        out_shape=(
            jax.ShapeDtypeStruct((sequences, local_heads, share, key_width), jnp.bfloat16),
            jax.ShapeDtypeStruct((sequences, local_heads, share), jnp.bfloat16),
        ),
        in_specs=[smem, smem] + [anywhere] * 9,
        out_specs=(vmem, vmem),
        scratch_shapes=[
            pltpu.VMEM((tp_size, sequences, positions, depth), jnp.bfloat16),
            pltpu.VMEM(key_matrix.shape, jnp.bfloat16),
            pltpu.VMEM(value_matrix.shape, jnp.bfloat16),
            pltpu.VMEM(gate_matrix.shape[::-1], jnp.bfloat16),
            pltpu.VMEM(extra_log_decay.shape, jnp.float32),
            pltpu.VMEM(next_token_query.shape, jnp.bfloat16),
            pltpu.VMEM(next_token_key.shape, jnp.bfloat16),
            pltpu.VMEM(next_token_value.shape, jnp.bfloat16),
            pltpu.VMEM(read_norm_gain.shape, jnp.float32),
            pltpu.VMEM((rows, key_total), jnp.float32),
            pltpu.VMEM((rows, value_total), jnp.float32),
            pltpu.VMEM((rows, gate_matrix.shape[1]), jnp.float32),
            pltpu.VMEM((sp_size, sequences, 2, positions, key_width), jnp.bfloat16),
            pltpu.VMEM((sp_size, sequences, 2, positions, key_width), jnp.bfloat16),
            pltpu.VMEM((sp_size, sequences, 8, positions), jnp.float32),
            pltpu.VMEM((sp_size, sequences, 8, positions), jnp.float32),
            pltpu.VMEM((sp_size, sequences, share, key_width), jnp.bfloat16),
            pltpu.VMEM((sp_size, sequences, share, key_width), jnp.bfloat16),
            pltpu.VMEM((sequences, 8, value_width), jnp.float32),
            pltpu.VMEM((sp_size, sequences, 8, value_width), jnp.float32),
            dma((sequences,)),
            dma((8,)),
            dma((tp_size, sequences)),
            dma((tp_size, sequences, 3)),
            dma((2, sequences, sp_size)),
            dma((2, sequences, sp_size)),
            dma((2, sequences)),
            dma((2, sequences, sp_size)),
            dma((2, sequences, sp_size)),
            dma((2, sequences)),
        ],
        compiler_params=pltpu.CompilerParams(
            collective_id=0, has_side_effects=True
        ),
    )(
        head_decay_rate,
        next_write_strength,
        tokens,
        key_matrix,
        value_matrix,
        gate_matrix.T,
        extra_log_decay,
        next_token_query,
        next_token_key,
        next_token_value,
        read_norm_gain,
    )
    return jnp.swapaxes(turned, 2, 3), read


def local(*arguments):
    tokens, key_matrix, value_matrix = arguments[:3]
    sequences, positions, _ = tokens.shape
    local_heads = arguments[4].shape[0]
    sp_size = lax.axis_size("sp")
    fits = (
        local_heads == sp_size
        and sequences == 2
        and lax.axis_size("tp") % CORES == 0
        and lax.axis_size("tp") > CORES
        and positions == key_matrix.shape[1] // local_heads
        and positions == value_matrix.shape[1] // local_heads
        and positions % 128 == 0
    )
    return local_fused(*arguments) if fits else local_general(*arguments)


def solution(mesh):
    in_specs = (
        P(None, "sp", "tp"),
        P(None, "tp"),
        P(None, "tp"),
        P(),
        P("tp"),
        P(None, "tp", "sp"),
        P(None, "tp"),
        P(None, "tp"),
        P(None, "tp", "sp"),
        P(None, "tp"),
        P("sp"),
    )
    out_specs = (P(None, "tp", None, "sp"), P(None, "tp", "sp"))
    return jax.shard_map(local, mesh=mesh, in_specs=in_specs, out_specs=out_specs, check_vma=False)
```
